32 devices in a mesh: sp: 8 (over z, y), tp: 4 (over x, core).
Axes of the slice: x: 2, y: 2, z: 4, core: 2. Of those that a mesh axis runs over, the one named last changes fastest.
Arguments:
- resid: bfloat16 [2048, 2048], P(('sp', 'tp')), may hold values from -0.3125 to 0.3125
- q_latent: bfloat16 [2048, 768], P('sp'), may hold values from -6 to 6
- kv_latent: bfloat16 [2048, 512], P('sp'), may hold values from -6 to 6
- rope_key: bfloat16 [2048, 32], P('sp'), may hold values from -6 to 6
- q_gain: float32 [768], replicated, may hold values from 0.6 to 10, as said below
- kv_gain: float32 [512], replicated, may hold values from 0.6 to 10
- w_q_small: bfloat16 [768, 768], P(None, 'tp'), may hold values from -0.21875 to 0.21875
- w_q_large: bfloat16 [768, 1280], P(None, 'tp'), may hold values from -0.21875 to 0.21875
- w_kv_small: bfloat16 [512, 1024], P(None, 'tp'), may hold values from -0.25 to 0.25
- w_kv_large: bfloat16 [512, 2048], P(None, 'tp'), may hold values from -0.25 to 0.25
- w_out_small: bfloat16 [512, 2048], P('tp'), may hold values from -0.15625 to 0.15625
- w_out_large: bfloat16 [1024, 2048], P('tp'), may hold values from -0.15625 to 0.15625
- ffn_gain: float32 [2048], replicated, may hold values from 0.1 to 1.9
- w_up: bfloat16 [2048, 8192], P('sp', 'tp'), may hold values from -0.125 to 0.125
- w_down: bfloat16 [8192, 2048], P('tp', 'sp'), may hold values from -0.0625 to 0.0625
Outputs:
- layer_out: bfloat16 [2048, 2048], P(('sp', 'tp'))
The draws below stay inside these ranges and needn't reach their ends.
Inputs may be any that keep to these rules, and one draw needn't show every extreme that they name: q_gain and kv_gain are positive.
All inputs are finite; a program needn't handle non-finite values.
Results may differ from the reference program's by a relative error of at most 0.025.
The reference program's roundings to bfloat16 on the way (of `query_normed`, `key_normed`, `key_rot`, `weights`, `after_attn`, `ffn_normed` and `hidden`) count: a program that leaves them out, or rounds other values in their place, can miss the bound.
Values may be sent and summed in bfloat16 or wider, within the bound.
No kernel may reach another device: no remote copies, remote signals or barrier semaphores. Data moves between devices by JAX's collectives and lax.ppermute only.
A program may use at most 128 MiB of HBM per device.

```python
import math
import jax
import jax.numpy as jnp
from jax import lax

WIDTH = 2048
MIXER_UNITS = 8192
QUERY_RANK = 768
LATENT_RANK = 512
HEADS_SMALL = 8
HEADS_LARGE = 8
SMALL_DIM = 64
LARGE_DIM = 128
ROPE_DIM = 32
TOKENS = 2048


def draw_q_gain(key, part):
    return jnp.exp(jax.random.uniform(key, (QUERY_RANK,), jnp.float32, -0.4, 0.4))


def draw_kv_gain(key, part):
    return jnp.exp(jax.random.uniform(key, (LATENT_RANK,), jnp.float32, -0.4, 0.4))


def block_levels(own_key, shape, shards, low, largest):
    factor_of, own = 1.0, jax.random.fold_in(own_key, 6)
    for position, shards_of in shards:
        heights = jnp.exp(jax.random.uniform(jax.random.fold_in(own, position), (shards_of,), jnp.float32, low / len(shards), largest / len(shards)))
        factor_of = factor_of * jnp.repeat(heights, shape[position] // shards_of).reshape([-1 if axis == position else 1 for axis in range(len(shape))])
    return factor_of


def normal_values(own_key, dims, width, limit, cuts=(), held_as=jnp.bfloat16):
    values = width * jax.random.normal(own_key, dims, jnp.float32)
    if cuts:
        values = values * block_levels(own_key, dims, cuts, -0.22, 0.18)
    return jnp.clip(values, -limit, limit).astype(held_as)


def setup_inputs(seed: int = 0) -> dict:
    arg_keys = jax.random.split(jax.random.key(seed), 16)
    return {
        "resid": normal_values(arg_keys[0], (TOKENS, WIDTH), 0.02, 0.3125, ((0, 32),)),
        "q_latent": normal_values(arg_keys[1], (TOKENS, QUERY_RANK), 1.0, 6.0, ((0, 8),)),
        "kv_latent": normal_values(arg_keys[2], (TOKENS, LATENT_RANK), 1.0, 6.0, ((0, 8),)),
        "rope_key": normal_values(arg_keys[3], (TOKENS, ROPE_DIM), 1.0, 6.0, ((0, 8),)),
        "q_gain": draw_q_gain(jax.random.fold_in(arg_keys[15], 71), 0),
        "kv_gain": draw_kv_gain(jax.random.fold_in(arg_keys[15], 71), 0),
        "w_q_small": normal_values(arg_keys[6], (QUERY_RANK, HEADS_SMALL * (SMALL_DIM + ROPE_DIM)), QUERY_RANK ** -0.5, 0.21875, ((1, 4),)),
        "w_q_large": normal_values(arg_keys[7], (QUERY_RANK, HEADS_LARGE * (LARGE_DIM + ROPE_DIM)), QUERY_RANK ** -0.5, 0.21875, ((1, 4),)),
        "w_kv_small": normal_values(arg_keys[8], (LATENT_RANK, HEADS_SMALL * 2 * SMALL_DIM), LATENT_RANK ** -0.5, 0.25, ((1, 4),)),
        "w_kv_large": normal_values(arg_keys[9], (LATENT_RANK, HEADS_LARGE * 2 * LARGE_DIM), LATENT_RANK ** -0.5, 0.25, ((1, 4),)),
        "w_out_small": normal_values(arg_keys[10], (HEADS_SMALL * SMALL_DIM, WIDTH), (HEADS_SMALL * SMALL_DIM + HEADS_LARGE * LARGE_DIM) ** -0.5, 0.15625, ((0, 4),)),
        "w_out_large": normal_values(arg_keys[11], (HEADS_LARGE * LARGE_DIM, WIDTH), (HEADS_SMALL * SMALL_DIM + HEADS_LARGE * LARGE_DIM) ** -0.5, 0.15625, ((0, 4),)),
        "ffn_gain": jnp.clip(1.0 + 0.18 * jax.random.normal(arg_keys[12], (WIDTH,), jnp.float32), 0.1, 1.9),
        "w_up": normal_values(arg_keys[13], (WIDTH, MIXER_UNITS), WIDTH ** -0.5, 0.125, ((0, 8), (1, 4))),
        "w_down": normal_values(arg_keys[14], (MIXER_UNITS, WIDTH), MIXER_UNITS ** -0.5, 0.0625, ((0, 4), (1, 8))),
    }


epsilon = 1e-06
theta_base = 10000.0

def rms_scale(inputs, gain_vec):
    values = inputs.astype(jnp.float32)
    return values * lax.rsqrt(lax.optimization_barrier(jnp.mean(values * values, axis=-1, keepdims=True)) + epsilon) * gain_vec

def rotary(values, positions):
    halfway = values.shape[-1] // 2
    inverse = theta_base ** (-jnp.arange(0, 2 * halfway, 2, dtype=jnp.float32) / (2 * halfway))
    angles = positions.astype(jnp.float32)[:, None] * inverse[None, :]
    cos_table = jnp.cos(angles)
    sin_table = jnp.sin(angles)
    if values.ndim == 3:
        cos_table = cos_table[:, None, :]
        sin_table = sin_table[:, None, :]
    first_half = values[..., :halfway]
    second_half = values[..., halfway:]
    return jnp.concatenate([first_half * cos_table - second_half * sin_table, second_half * cos_table + first_half * sin_table], axis=-1)

def queries(normed, weight, nope_dim, positions):
    projected = jnp.dot(normed, weight, preferred_element_type=jnp.float32)
    projected = projected.reshape(projected.shape[0], -1, nope_dim + ROPE_DIM)
    turned = rotary(projected[..., nope_dim:], positions)
    return jnp.concatenate([projected[..., :nope_dim], turned], axis=-1).astype(jnp.bfloat16)

def group_attention(query_rows, keys_values, key_rot, nope_dim):
    length = query_rows.shape[0]
    head_count = query_rows.shape[1]
    block_rows = math.gcd(length, 512)
    block_count = length // block_rows
    key_part = keys_values[..., :nope_dim].astype(jnp.float32)
    value_part = keys_values[..., nope_dim:].astype(jnp.float32)
    rot_f32 = key_rot.astype(jnp.float32)
    score_scale = (nope_dim + ROPE_DIM) ** (-0.5)
    key_pos = jnp.arange(length, dtype=jnp.int32)

    def attend_block(block_args):
        query_block, block_index = block_args
        query_f32 = query_block.astype(jnp.float32)
        scores = jnp.einsum('qhd,khd->hqk', query_f32[..., :nope_dim], key_part)
        scores = scores + jnp.einsum('qhr,kr->hqk', query_f32[..., nope_dim:], rot_f32)
        scores = scores * score_scale
        query_pos = block_index * block_rows + jnp.arange(block_rows, dtype=jnp.int32)
        causal = key_pos[None, :] <= query_pos[:, None]
        scores = jnp.where(causal[None], scores, -jnp.inf)
        row_max = lax.optimization_barrier(jnp.max(scores, axis=-1, keepdims=True))
        exponent = jnp.exp(scores - row_max)
        row_sum = lax.optimization_barrier(jnp.sum(exponent, axis=-1))
        weights = lax.optimization_barrier(exponent.astype(jnp.bfloat16)).astype(jnp.float32)
        summed = jnp.einsum('hqk,khd->qhd', weights, value_part)
        return (summed / jnp.transpose(row_sum)[:, :, None]).astype(jnp.bfloat16)
    blocks = query_rows.reshape(block_count, block_rows, head_count, query_rows.shape[-1])
    result = lax.map(attend_block, (blocks, jnp.arange(block_count, dtype=jnp.int32)))
    return result.reshape(length, -1)

def reference(resid, q_latent, kv_latent, rope_key, q_gain, kv_gain, w_q_small, w_q_large, w_kv_small, w_kv_large, w_out_small, w_out_large, ffn_gain, w_up, w_down):
    positions = jnp.arange(TOKENS, dtype=jnp.int32)
    query_normed = rms_scale(q_latent, q_gain).astype(jnp.bfloat16)
    key_normed = rms_scale(kv_latent, kv_gain).astype(jnp.bfloat16)
    key_rot = rotary(rope_key.astype(jnp.float32), positions).astype(jnp.bfloat16)
    query_small = queries(query_normed, w_q_small, SMALL_DIM, positions)
    query_large = queries(query_normed, w_q_large, LARGE_DIM, positions)
    kv_small = jnp.dot(key_normed, w_kv_small, preferred_element_type=jnp.float32).astype(jnp.bfloat16)
    kv_small = kv_small.reshape(TOKENS, HEADS_SMALL, 2 * SMALL_DIM)
    kv_large = jnp.dot(key_normed, w_kv_large, preferred_element_type=jnp.float32).astype(jnp.bfloat16)
    kv_large = kv_large.reshape(TOKENS, HEADS_LARGE, 2 * LARGE_DIM)
    attn_small = group_attention(query_small, kv_small, key_rot, SMALL_DIM)
    attn_large = group_attention(query_large, kv_large, key_rot, LARGE_DIM)
    mixed_rows = jnp.dot(attn_small, w_out_small, preferred_element_type=jnp.float32)
    mixed_rows = mixed_rows + jnp.dot(attn_large, w_out_large, preferred_element_type=jnp.float32)
    after_attn = (resid.astype(jnp.float32) + mixed_rows).astype(jnp.bfloat16)
    ffn_normed = rms_scale(after_attn, ffn_gain).astype(jnp.bfloat16)
    hidden = jnp.square(jax.nn.relu(jnp.dot(ffn_normed, w_up, preferred_element_type=jnp.float32)))
    hidden = hidden.astype(jnp.bfloat16)
    ffn_rows = jnp.dot(hidden, w_down, preferred_element_type=jnp.float32)
    return (after_attn.astype(jnp.float32) + ffn_rows).astype(jnp.bfloat16)
```

```python
import functools

import jax
import jax.numpy as jnp
from jax import lax
from jax.experimental import pallas as pl
from jax.experimental.pallas import tpu as pltpu
from jax.sharding import PartitionSpec as P

SMALL_DIM = 64
LARGE_DIM = 128
ROPE_DIM = 32
LANES = 128
LOG2E = 1.4426950408889634

epsilon = 1e-06
theta_base = 10000.0
mask_floor = -1e30


VMEM = pl.BlockSpec(memory_space=pltpu.VMEM)
SMEM = pl.BlockSpec(memory_space=pltpu.SMEM)
HBM = pl.BlockSpec(memory_space=pltpu.HBM)


def nt_dot(a, b):
    return lax.dot_general(a, b, (((1,), (1,)), ((), ())), preferred_element_type=jnp.float32)


def rms(values, gain):
    scale = lax.rsqrt(jnp.mean(values * values, axis=-1, keepdims=True) + epsilon)
    return values * scale * gain


def turn(tile, cos_tile, sin_tile):
    half = ROPE_DIM // 2
    lane = lax.broadcasted_iota(jnp.int32, tile.shape, 1)
    other = jnp.where(
        lane < half, pltpu.roll(tile, LANES - half, 1), pltpu.roll(tile, half, 1)
    )
    return tile * cos_tile + other * sin_tile


def prep_kernel(place_ref, latent_ref, gain_ref, rope_ref, cos_ref, sin_ref, packed_ref):
    rows = packed_ref.shape[0] * 16 // 17
    start = pl.multiple_of(place_ref[1] * rows, rows)
    latent = latent_ref[pl.ds(start, rows), :].astype(jnp.float32)
    packed_ref[:rows, :] = rms(latent, gain_ref[...]).astype(jnp.bfloat16)
    rope = rope_ref[pl.ds(start, rows), :].astype(jnp.float32)
    rope = jnp.concatenate(
        [rope, jnp.zeros((rows, LANES - ROPE_DIM), jnp.float32)], axis=1
    )
    turned = turn(rope, cos_ref[pl.ds(start, rows), :], sin_ref[pl.ds(start, rows), :])
    group = rows // 16
    per_tile = LANES // ROPE_DIM
    tiles = []
    for tile in range(16 // per_tile):
        total = turned[tile * per_tile * group : (tile * per_tile + 1) * group]
        for q in range(1, per_tile):
            first = (tile * per_tile + q) * group
            total = total + pltpu.roll(turned[first : first + group], q * ROPE_DIM, 1)
        tiles.append(total)
    packed_ref[rows:, :] = jnp.concatenate(tiles, axis=1).astype(jnp.bfloat16)


def unpack_rope(packed):
    packed = packed.astype(jnp.float32)
    per_tile = LANES // ROPE_DIM
    pieces = []
    for g in range(16):
        tile = packed[:, (g // per_tile) * LANES : (g // per_tile + 1) * LANES]
        shift = (g % per_tile) * ROPE_DIM
        pieces.append(pltpu.roll(tile, LANES - shift, 1) if shift else tile)
    return jnp.concatenate(pieces, axis=0).astype(jnp.bfloat16)


def attention_kernel(
    small_heads,
    large_heads,
    place_ref,
    latent_ref,
    gain_ref,
    wq_ref,
    cos_ref,
    sin_ref,
    first_ref,
    second_ref,
    wkv_small_ref,
    wkv_large_ref,
    out_ref,
    query_ref,
    max_ref,
    sum_ref,
    acc_ref,
):
    heads = small_heads + large_heads
    rows = latent_ref.shape[0]
    half = first_ref.shape[1] * 16 // 17
    own_sp, own_half = place_ref[0], place_ref[1]
    normed = rms(latent_ref[...].astype(jnp.float32), gain_ref[...]).astype(jnp.bfloat16)
    for h in range(heads):
        projected = jnp.dot(
            normed, wq_ref[:, 2 * LANES * h : 2 * LANES * (h + 1)],
            preferred_element_type=jnp.float32,
        )
        query_ref[h, :, :LANES] = projected[:, :LANES].astype(jnp.bfloat16)
        query_ref[h, :, LANES:] = turn(projected[:, LANES:], cos_ref[...], sin_ref[...]).astype(
            jnp.bfloat16
        )

    def block_heads(j):
        latent = jnp.concatenate([first_ref[j, :half, :], second_ref[j, :half, :]], axis=0)
        rope = jnp.concatenate(
            [unpack_rope(first_ref[j, half:, :]), unpack_rope(second_ref[j, half:, :])], axis=0
        )
        small = jnp.dot(latent, wkv_small_ref[...], preferred_element_type=jnp.float32)
        large = jnp.dot(latent, wkv_large_ref[...], preferred_element_type=jnp.float32)
        small = small.astype(jnp.bfloat16)
        large = large.astype(jnp.bfloat16)
        for h in range(heads):
            if h < small_heads:
                keys = values = small[:, LANES * h : LANES * (h + 1)]
                width = SMALL_DIM + ROPE_DIM
            else:
                first = 2 * LANES * (h - small_heads)
                keys = large[:, first : first + LANES]
                values = large[:, first + LANES : first + 2 * LANES]
                width = LARGE_DIM + ROPE_DIM
            scores = nt_dot(jnp.concatenate([keys, rope], axis=1), query_ref[h])
            yield h, scores, values, width**-0.5 * LOG2E

    def weigh(weights, values):
        return lax.dot_general(
            values, weights.astype(jnp.bfloat16), (((0,), (0,)), ((), ())),
            preferred_element_type=jnp.float32,
        )

    key_row = lax.broadcasted_iota(jnp.int32, (rows, rows), 0)
    key_pos = jnp.where(
        key_row < half, key_row + own_half * half, key_row - half + (1 - own_half) * half
    )
    causal = key_pos <= lax.broadcasted_iota(jnp.int32, (rows, rows), 1)
    for h, scores, values, factor in block_heads(own_sp):
        scores = jnp.where(causal, scores, mask_floor)
        top = jnp.max(scores, axis=0, keepdims=True)
        weights = jnp.where(causal, jnp.exp2((scores - top) * factor), 0.0)
        max_ref[h] = top
        sum_ref[h] = jnp.sum(weights, axis=0, keepdims=True)
        acc_ref[h] = weigh(weights, values)

    @pl.loop(0, own_sp)
    def _(j):
        for h, scores, values, factor in block_heads(j):
            old = max_ref[h]
            top = jnp.maximum(old, jnp.max(scores, axis=0, keepdims=True))
            shrink = jnp.exp2((old - top) * factor)
            weights = jnp.exp2((scores - top) * factor)
            max_ref[h] = top
            sum_ref[h] = sum_ref[h] * shrink + jnp.sum(weights, axis=0, keepdims=True)
            acc_ref[h] = acc_ref[h] * shrink + weigh(weights, values)

    parts = []
    for h in range(heads):
        result = acc_ref[h] / sum_ref[h]
        parts.append(result[SMALL_DIM:] if h < small_heads else result)
    out_ref[...] = jnp.transpose(jnp.concatenate(parts, axis=0)).astype(jnp.bfloat16)


def mixed_kernel(count, place_ref, attn_ref, resid_ref, gain_ref, *refs):
    weights, (after_ref, normed_ref) = refs[:count], refs[count:]
    own = place_ref[2]
    total = resid_ref[...].astype(jnp.float32)
    mixed = None
    for k in range(count):
        part = jnp.dot(attn_ref[own ^ k], weights[k][...], preferred_element_type=jnp.float32)
        mixed = part if mixed is None else mixed + part
    after = (total + mixed).astype(jnp.bfloat16)
    after_ref[...] = after
    normed_ref[...] = rms(after.astype(jnp.float32), gain_ref[...]).astype(jnp.bfloat16)


def mixer_kernel(n_x, n_up, n_down, place_ref, *refs):
    xs, refs = refs[:n_x], refs[n_x:]
    ups, refs = refs[:n_up], refs[n_up:]
    downs, refs = refs[:n_down], refs[n_down:]
    keep_ref, send_ref, x_all, up_all, down_all, hidden, sems = refs
    own = place_ref[0]
    copies = []
    for k, ref in enumerate(xs):
        rows = ref.shape[0]
        copies.append((ref, x_all.at[k * rows : (k + 1) * rows, :]))
    for k, ref in enumerate(ups):
        rows = ref.shape[0]
        start = pl.multiple_of((own ^ k) * rows, rows)
        copies.append((ref, up_all.at[pl.ds(start, rows), :]))
    for k, ref in enumerate(downs):
        columns = ref.shape[1]
        start = pl.multiple_of((own ^ k) * columns, columns) if n_down > 1 else 0
        copies.append((ref, down_all.at[:, pl.ds(start, columns)]))
    copies = [
        pltpu.make_async_copy(source, target, sems.at[i])
        for i, (source, target) in enumerate(copies)
    ]
    for copy in copies:
        copy.start()
    for copy in copies[: n_x + n_up]:
        copy.wait()
    step = 256

    @pl.loop(0, hidden.shape[1] // step)
    def _(n):
        at = pl.ds(pl.multiple_of(n * step, step), step)
        projected = jnp.dot(x_all[...], up_all[:, at], preferred_element_type=jnp.float32)
        hidden[:, at] = jnp.square(jnp.maximum(projected, 0.0)).astype(jnp.bfloat16)

    for copy in copies[n_x + n_up :]:
        copy.wait()
    rows = keep_ref.shape[0]

    @pl.loop(0, down_all.shape[1] // step)
    def _(n):
        at = pl.ds(pl.multiple_of(n * step, step), step)
        result = jnp.dot(hidden[...], down_all[:, at], preferred_element_type=jnp.float32)
        keep_ref[:, at] = result[:rows].astype(jnp.bfloat16)
        send_ref[:, at] = result[rows:].astype(jnp.bfloat16)


def bits_of(count):
    return [1 << i for i in range(count.bit_length() - 1)]


def on_device(
    n_sp,
    n_tp,
    resid,
    q_latent,
    kv_latent,
    rope_key,
    q_gain,
    kv_gain,
    w_q_small,
    w_q_large,
    w_kv_small,
    w_kv_large,
    w_out_small,
    w_out_large,
    ffn_gain,
    w_up,
    w_down,
):
    bf16, f32 = jnp.bfloat16, jnp.float32
    tok_rows = q_latent.shape[0]
    own_rows, width = resid.shape
    sp = lax.axis_index("sp")
    tp = lax.axis_index("tp")
    place = jnp.stack([sp, tp & 1, tp]).astype(jnp.int32)

    def swap(value, sp_bits=0, tp_bits=0):
        pairs = [
            (s * n_tp + t, (s ^ sp_bits) * n_tp + (t ^ tp_bits))
            for s in range(n_sp)
            for t in range(n_tp)
        ]
        return lax.ppermute(value, ("sp", "tp"), pairs)

    top_bit = n_sp // 2
    low_bits = bits_of(top_bit)
    tp_bits = bits_of(n_tp)

    half = ROPE_DIM // 2
    inverse = theta_base ** (-jnp.arange(0, ROPE_DIM, 2, dtype=f32) / ROPE_DIM)
    positions = (sp * tok_rows + jnp.arange(tok_rows, dtype=jnp.int32)).astype(f32)
    angles = positions[:, None] * inverse[None, :]
    cosine, sine = jnp.cos(angles), jnp.sin(angles)
    blank = jnp.zeros((tok_rows, LANES - ROPE_DIM), f32)
    cos_table = jnp.concatenate([cosine, cosine, blank], axis=1)
    sin_table = jnp.concatenate([-sine, sine, blank], axis=1)

    half_rows = tok_rows // 2
    packed = pl.pallas_call(
        prep_kernel,
        name="prep",
        out_shape=jax.ShapeDtypeStruct((half_rows * 17 // 16, kv_latent.shape[1]), bf16),
        in_specs=[SMEM] + [VMEM] * 5,
        out_specs=VMEM,
    )(place, kv_latent, kv_gain[None], rope_key, cos_table, sin_table)
    first = lax.all_to_all(
        jnp.broadcast_to(packed[None], (n_sp,) + packed.shape), "sp", 0, 0
    )
    second = swap(first, tp_bits=1)

    units = w_up.shape[1] // 2
    upper = jnp.where(sp >= top_bit, 1, 0)
    ups = {
        0: lax.dynamic_slice_in_dim(w_up, upper * units, units, 1),
        top_bit: swap(lax.dynamic_slice_in_dim(w_up, (1 - upper) * units, units, 1), top_bit),
    }
    downs = {
        0: lax.dynamic_slice_in_dim(w_down, upper * units, units, 0),
        top_bit: swap(lax.dynamic_slice_in_dim(w_down, (1 - upper) * units, units, 0), top_bit),
    }
    for bit in low_bits:
        ups.update({k | bit: swap(v, bit) for k, v in ups.items()})
    for bit in reversed(low_bits):
        downs.update({k | bit: swap(v, bit) for k, v in downs.items()})
    up_list = [ups[k] for k in range(n_sp)]
    down_list = [downs[k] for k in range(n_sp)]
    if w_down.shape[1] % LANES:
        ordered = jnp.stack(down_list)[jnp.arange(n_sp) ^ sp]
        down_list = [jnp.transpose(ordered, (1, 0, 2)).reshape(units, width)]

    outs = [jnp.concatenate([w_out_small, w_out_large], axis=0)]
    for bit in reversed(tp_bits):
        outs = outs + [swap(v, tp_bits=bit) for v in outs]
    order = [0]
    for bit in reversed(tp_bits):
        order = order + [k | bit for k in order]
    out_list = [outs[order.index(k)] for k in range(n_tp)]

    def padded_heads(weight, nope_dim):
        weight = weight.reshape(weight.shape[0], -1, nope_dim + ROPE_DIM)
        content = jnp.pad(weight[..., :nope_dim], ((0, 0), (0, 0), (0, LANES - nope_dim)))
        rope = jnp.pad(weight[..., nope_dim:], ((0, 0), (0, 0), (0, LANES - ROPE_DIM)))
        return jnp.concatenate([content, rope], axis=-1).reshape(weight.shape[0], -1)

    small_heads = w_q_small.shape[1] // (SMALL_DIM + ROPE_DIM)
    large_heads = w_q_large.shape[1] // (LARGE_DIM + ROPE_DIM)
    heads = small_heads + large_heads
    w_q = jnp.concatenate(
        [padded_heads(w_q_small, SMALL_DIM), padded_heads(w_q_large, LARGE_DIM)], axis=1
    )
    attn_width = small_heads * SMALL_DIM + large_heads * LARGE_DIM
    attn = pl.pallas_call(
        functools.partial(attention_kernel, small_heads, large_heads),
        name="attention",
        out_shape=jax.ShapeDtypeStruct((tok_rows, attn_width), bf16),
        in_specs=[SMEM] + [VMEM] * 9,
        out_specs=VMEM,
        scratch_shapes=[
            pltpu.VMEM((heads, tok_rows, 2 * LANES), bf16),
            pltpu.VMEM((heads, 1, tok_rows), f32),
            pltpu.VMEM((heads, 1, tok_rows), f32),
            pltpu.VMEM((heads, LANES, tok_rows), f32),
        ],
        cost_estimate=pl.CostEstimate(
            flops=10_000_000_000, bytes_accessed=8_000_000, transcendentals=2_000_000
        ),
    )(
        place,
        q_latent,
        q_gain[None],
        w_q,
        cos_table,
        sin_table,
        first,
        second,
        w_kv_small,
        w_kv_large,
    )
    attn = lax.all_to_all(attn.reshape(n_tp, own_rows, attn_width), "tp", 0, 0)
    after_attn, ffn_normed = pl.pallas_call(
        functools.partial(mixed_kernel, n_tp),
        name="out_proj",
        out_shape=[jax.ShapeDtypeStruct((own_rows, width), bf16)] * 2,
        in_specs=[SMEM] + [VMEM] * (3 + n_tp),
        out_specs=[VMEM] * 2,
        cost_estimate=pl.CostEstimate(
            flops=4_000_000_000, bytes_accessed=8_000_000, transcendentals=0
        ),
    )(place, attn, resid, ffn_gain[None], *out_list)

    rows_list = [ffn_normed, swap(ffn_normed, top_bit)]
    for bit in reversed(tp_bits):
        rows_list = rows_list + [swap(v, tp_bits=bit) for v in rows_list]
    group_rows = own_rows * len(rows_list)
    n_x, n_up, n_down = len(rows_list), len(up_list), len(down_list)
    keep, send = pl.pallas_call(
        functools.partial(mixer_kernel, n_x, n_up, n_down),
        name="mixer",
        out_shape=[jax.ShapeDtypeStruct((group_rows // 2, width), bf16)] * 2,
        in_specs=[SMEM] + [HBM] * (n_x + n_up + n_down),
        out_specs=[VMEM] * 2,
        scratch_shapes=[
            pltpu.VMEM((group_rows, width), bf16),
            pltpu.VMEM((width, units), bf16),
            pltpu.VMEM((units, width), bf16),
            pltpu.VMEM((group_rows, units), bf16),
            pltpu.SemaphoreType.DMA((n_x + n_up + n_down,)),
        ],
        cost_estimate=pl.CostEstimate(
            flops=8_000_000_000, bytes_accessed=12_000_000, transcendentals=0
        ),
    )(place, *rows_list, *up_list, *down_list)

    for bit in tp_bits:
        total = (keep.astype(f32) + swap(send, tp_bits=bit).astype(f32)).astype(bf16)
        count = total.shape[0] // 2
        keep, send = total[:count], total[count:]
    got = swap(send, top_bit)
    ffn_rows = keep.astype(f32) + got.astype(f32)
    return (after_attn.astype(f32) + ffn_rows).astype(bf16)


def solution(mesh):
    n_sp, n_tp = mesh.shape["sp"], mesh.shape["tp"]
    return jax.shard_map(
        functools.partial(on_device, n_sp, n_tp),
        mesh=mesh,
        in_specs=(
            P(("sp", "tp"), None),
            P("sp", None),
            P("sp", None),
            P("sp", None),
            P(),
            P(),
            P(None, "tp"),
            P(None, "tp"),
            P(None, "tp"),
            P(None, "tp"),
            P("tp", None),
            P("tp", None),
            P(),
            P("sp", "tp"),
            P("tp", "sp"),
        ),
        out_specs=P(("sp", "tp"), None),
        check_vma=False,
    )
```
